32 devices in a mesh: ra: 8 (over z, y), cb: 4 (over x, core).
Axes of the slice: x: 2, y: 2, z: 4, core: 2. Of those that a mesh axis runs over, the one named last changes fastest.
Arguments:
- tokens: bfloat16 [512, 4096], P(None, 'cb'), may hold values from -82 to 82
- gate_weight: float32 [2, 4096, 11264], P(None, 'cb', 'ra'), may hold values from -0.09375 to 0.09375
- up_weight: float32 [2, 4096, 11264], P(None, 'cb', 'ra'), may hold values from -0.09375 to 0.09375
- down_weight: float32 [2, 11264, 4096], P(None, 'ra', 'cb'), may hold values from -0.0546875 to 0.0546875
- gate_scale: float32 [2, 11264], P(None, 'ra'), may hold values from 0.5 to 2
- up_scale: float32 [2, 11264], P(None, 'ra'), may hold values from 0.5 to 2
- down_scale: float32 [2, 4096], P(None, 'cb'), may hold values from 0.5 to 2
- norm_gain: float32 [2, 4096], P(None, 'cb'), may hold values from 0.1 to 1.9
- conv_taps: float32 [2, 3, 11264], P(None, None, 'ra'), may hold values from -3 to 3
- conv_bias: float32 [2, 11264], P(None, 'ra'), may hold values from -3 to 3
Outputs:
- layer_out: bfloat16 [512, 4096], P(None, 'cb')
The draws below stay inside these ranges and needn't reach their ends.
All inputs are finite; a program needn't handle non-finite values.
Results may differ from the reference program's by a relative error of at most 0.012.
Values may be sent and summed in bfloat16 or wider, within the bound.
A program may use at most 128 MiB of HBM per device.

```python
import math
import jax
import jax.numpy as jnp
from jax import lax

D = 4096
FF = 11264
TOKENS = 512
LAYERS = 2
KERNEL = 3


def draw_tokens(key, part):
    k_base, k_row, k_col = jax.random.split(key, 3)
    trend = jnp.linspace(0.0, math.log(10.0), D)
    jitter = jax.random.uniform(k_col, (D,), jnp.float32, -0.3, 0.3)
    column = jnp.exp(trend + jitter)
    row_scale = jnp.exp(jax.random.uniform(k_row, (TOKENS, 1), jnp.float32, 0.0, math.log(10.0)))
    base = jnp.clip(jax.random.normal(k_base, (TOKENS, D), jnp.float32), -6.0, 6.0)
    values = base * row_scale * column * 0.1
    return values.astype(jnp.bfloat16)


def level_of(own_key, shape, cuts, least, high):
    level, own = 1.0, jax.random.fold_in(own_key, 6)
    for axis_at, parts in cuts:
        steps = jnp.exp(jax.random.uniform(jax.random.fold_in(own, axis_at), (parts,), jnp.float32, least / len(cuts), high / len(cuts)))
        level = level * jnp.repeat(steps, shape[axis_at] // parts).reshape([-1 if axis == axis_at else 1 for axis in range(len(shape))])
    return level


def normal_values(stream_key, shape, width, bound, cuts=(), dtype=jnp.bfloat16):
    array = jax.random.normal(stream_key, shape, jnp.float32) * width
    if len(cuts) > 0:
        array = level_of(stream_key, shape, cuts, -0.22, 0.18) * array
    return jnp.clip(array, min=-bound, max=bound).astype(dtype)


def setup_inputs(seed: int = 0) -> dict:
    streams_of = jax.random.split(jax.random.key(seed), 11)
    return {
        "tokens": draw_tokens(jax.random.fold_in(streams_of[10], 71), 0),
        "gate_weight": normal_values(streams_of[1], (LAYERS, D, FF), D ** -0.5, 0.09375, ((1, 4), (2, 8)), jnp.float32),
        "up_weight": normal_values(streams_of[2], (LAYERS, D, FF), D ** -0.5, 0.09375, ((1, 4), (2, 8)), jnp.float32),
        "down_weight": normal_values(streams_of[3], (LAYERS, FF, D), FF ** -0.5, 0.0546875, ((1, 8), (2, 4)), jnp.float32),
        "gate_scale": jnp.clip(jnp.exp(math.log(2.0) - 1.3862944 * jax.random.uniform(streams_of[4], (LAYERS, FF), jnp.float32) ** level_of(streams_of[4], (LAYERS, FF), ((1, 8),), -0.2, 0.2)), 0.5, 2.0),
        "up_scale": jnp.clip(jnp.exp(math.log(2.0) - 1.3862944 * jax.random.uniform(streams_of[5], (LAYERS, FF), jnp.float32) ** level_of(streams_of[5], (LAYERS, FF), ((1, 8),), -0.2, 0.2)), 0.5, 2.0),
        "down_scale": jnp.clip(jnp.exp(math.log(2.0) - 1.3862944 * jax.random.uniform(streams_of[6], (LAYERS, D), jnp.float32) ** level_of(streams_of[6], (LAYERS, D), ((1, 4),), -0.2, 0.2)), 0.5, 2.0),
        "norm_gain": jnp.clip(1.0 + 0.18 * jax.random.normal(streams_of[7], (LAYERS, D), jnp.float32), 0.1, 1.9),
        "conv_taps": normal_values(streams_of[8], (LAYERS, KERNEL, FF), 0.6, 3.0, ((2, 8),), jnp.float32),
        "conv_bias": normal_values(streams_of[9], (LAYERS, FF), 0.5, 3.0, ((1, 8),), jnp.float32),
    }


norm_eps = 1e-06
residual_scale = 0.25

def reference(tokens, gate_weight, up_weight, down_weight, gate_scale, up_scale, down_scale, norm_gain, conv_taps, conv_bias):
    hstate = tokens
    for layer in range(LAYERS):
        wide = hstate.astype(jnp.float32)
        stat = lax.optimization_barrier(jnp.mean(wide * wide, axis=1, keepdims=True))
        rscale = lax.rsqrt(stat + norm_eps)
        operand = (wide * norm_gain[layer]).astype(jnp.bfloat16)
        gate = jnp.dot(operand, gate_weight[layer].astype(jnp.bfloat16), preferred_element_type=jnp.float32) * rscale * gate_scale[layer]
        upward = jnp.dot(operand, up_weight[layer].astype(jnp.bfloat16), preferred_element_type=jnp.float32) * rscale * up_scale[layer]
        taps = conv_taps[layer]
        padded = jnp.pad(gate, ((1, 1), (0, 0)))
        mixed = taps[0] * padded[:-2] + taps[1] * padded[1:-1] + taps[2] * padded[2:] + conv_bias[layer]
        hidden = (jax.nn.silu(mixed) * upward).astype(jnp.bfloat16)
        branch = jnp.dot(hidden, down_weight[layer].astype(jnp.bfloat16), preferred_element_type=jnp.float32) * down_scale[layer]
        hstate = (residual_scale * wide + branch).astype(jnp.bfloat16)
    return hstate
```

```python
import functools

import jax
import jax.numpy as jnp
from jax import lax
from jax.experimental import pallas as pl
from jax.experimental.pallas import tpu as pltpu
from jax.sharding import PartitionSpec as P

MESH = pl.DeviceIdType.MESH
norm_eps = 1e-06
residual_scale = 0.25
LANES = 128
LAG = 3


def kernel(
    sizes,
    tok,
    gw_hbm,
    uw_hbm,
    dw_hbm,
    gs,
    us,
    ds_,
    gain,
    taps,
    bias,
    out,
    gw,
    uw,
    dw,
    dwb,
    operand,
    rsb,
    stat,
    part,
    crecv,
    xsend,
    xrecv,
    hid,
    ysend,
    own,
    yrecv,
    zsend,
    zrecv,
    hnew,
    wsem,
    ssem,
    csem,
    xsem,
    hsem,
    ysem,
    zsem,
    asem,
    fsem,
):
    layers, n_tok, d_loc, f_loc, d_all, n_z = sizes
    tiles = f_loc // LANES
    half, quarter = n_tok // 2, n_tok // 4
    zrows = half // n_z
    f32, bf16 = jnp.float32, jnp.bfloat16
    ra, cb = lax.axis_index("ra"), lax.axis_index("cb")
    z, y = ra // 2, ra % 2
    x, c = cb // 2, cb % 2
    core_dev = (ra, x * 2 + (1 - c))
    x_dev = (ra, (1 - x) * 2 + c)
    y_dev = (z * 2 + (1 - y), cb)

    def z_dev(k):
        return (lax.rem(z + k, n_z) * 2 + y, cb)

    def remote(src, dst, sems, dev):
        return pltpu.make_async_remote_copy(
            src_ref=src, dst_ref=dst, send_sem=sems[0], recv_sem=sems[1], device_id=dev, device_id_type=MESH
        )

    def load(l, n):
        src, dst = ((gw_hbm, gw), (uw_hbm, uw), (dw_hbm, dw))[n]
        return pltpu.make_async_copy(src.at[l], dst.at[l], wsem.at[l, n])

    load(0, 0).start()
    load(0, 1).start()

    barrier = pltpu.get_barrier_semaphore()
    peers = [(ra, lax.rem(cb + k, 4)) for k in range(1, 4)] + [y_dev] + [z_dev(k) for k in range(1, n_z)]
    for dev in peers:
        pl.semaphore_signal(barrier, inc=1, device_id=dev, device_id_type=MESH)
    pl.semaphore_wait(barrier, len(peers))

    my_rows = pl.ds(pl.multiple_of(c * half + x * quarter, quarter), quarter)
    x_rows = pl.ds(pl.multiple_of(c * half + (1 - x) * quarter, quarter), quarter)
    peer_half = pl.ds(pl.multiple_of((1 - c) * half, half), half)

    def zr(zz):
        return pl.ds(pl.multiple_of(zz * zrows, zrows), zrows)

    def hr(yy, zz):
        return pl.ds(pl.multiple_of(yy * half + zz * zrows, zrows), zrows)

    for l in range(layers):
        h = tok if l == 0 else hnew.at[l - 1]
        wide = h[...].astype(f32)
        ssq = jnp.sum(wide * wide, axis=1, keepdims=True)
        lane = lax.broadcasted_iota(jnp.int32, (n_tok, LANES), 1)
        row = lax.broadcasted_iota(jnp.int32, (n_tok, LANES), 0)
        pick = lane == lax.shift_right_logical(row, 3)
        packed = jnp.where(pick, jnp.broadcast_to(ssq, (n_tok, LANES)), 0.0)
        stat[l, 0] = jnp.sum(packed.reshape(n_tok // 8, 8, LANES), axis=0)
        for k in range(1, 4):
            remote(
                stat.at[l, 0], stat.at[l, k], (ssem.at[0, l, k - 1], ssem.at[1, l, k - 1]), (ra, lax.rem(cb + k, 4))
            ).start()
        operand[...] = (h[...].astype(f32) * gain[l : l + 1, :]).astype(bf16)
        if l == 0:
            load(0, 0).wait()
            load(0, 1).wait()
            load(0, 2).start()
            for ll in range(1, layers):
                for n in range(3):
                    load(ll, n).start()
        else:
            load(l, 0).wait()
            load(l, 1).wait()
        for k in range(1, 4):
            remote(
                stat.at[l, 0], stat.at[l, k], (ssem.at[0, l, k - 1], ssem.at[1, l, k - 1]), (ra, lax.rem(cb + k, 4))
            ).wait()
        total = stat[l, 0] + stat[l, 1] + stat[l, 2] + stat[l, 3]
        spread = jnp.broadcast_to(total[None], (n_tok // 8, 8, LANES)).reshape(n_tok, LANES)
        summed = jnp.sum(jnp.where(pick, spread, 0.0), axis=1, keepdims=True)
        rsb[...] = jnp.broadcast_to(lax.rsqrt(summed / d_all + norm_eps), (n_tok, LANES))

        def core_copy(j):
            return remote(
                part.at[j, peer_half, :], crecv.at[l, j], (csem.at[0, l, j], csem.at[1, l, j]), core_dev
            )

        def x_copy(j):
            return remote(xsend.at[j], xrecv.at[l, j], (xsem.at[0, l, j], xsem.at[1, l, j]), x_dev)

        x_local = pl.ds(pl.multiple_of((1 - x) * quarter, quarter), quarter)
        m_local = pl.ds(pl.multiple_of(x * quarter, quarter), quarter)

        def gate_step(j, carry):
            @pl.when(j < tiles)
            def _():
                cols = pl.ds(pl.multiple_of(j * LANES, LANES), LANES)
                w = jnp.concatenate([gw[l, :, cols].astype(bf16), uw[l, :, cols].astype(bf16)], axis=1)
                acc = jnp.dot(operand[...], w, preferred_element_type=f32)
                rs = rsb[...]
                g = acc[:, :LANES] * rs * gs[l : l + 1, cols]
                rows = lax.broadcasted_iota(jnp.int32, g.shape, 0)
                prev = jnp.where(rows == 0, 0.0, pltpu.roll(g, 1, 0))
                nxt = jnp.where(rows == n_tok - 1, 0.0, pltpu.roll(g, n_tok - 1, 0))
                mixed = taps[l, 0:1, cols] * prev + taps[l, 1:2, cols] * g + taps[l, 2:3, cols] * nxt
                part[j, :, 0:LANES] = mixed.astype(bf16)
                part[j, :, LANES : 2 * LANES] = (acc[:, LANES:] * rs * us[l : l + 1, cols]).astype(bf16)
                core_copy(j).start()

            @pl.when(j >= LAG)
            def _():
                i = j - LAG
                core_copy(i).wait_recv()
                xsend[i] = (part[i, x_rows, :].astype(f32) + crecv[l, i, x_local, :].astype(f32)).astype(bf16)
                x_copy(i).start()

            return carry

        lax.fori_loop(0, tiles + LAG, gate_step, 0)

        load(l, 2).wait()

        def cast_step(i, carry):
            r = pl.ds(pl.multiple_of(i * LANES, LANES), LANES)
            dwb[r, :] = dw[l, r, :].astype(bf16)
            return carry

        lax.fori_loop(0, tiles, cast_step, 0)

        def h_copy(j, n):
            cols = pl.ds(pl.multiple_of(j * LANES, LANES), LANES)
            block = hid.at[l, x_rows if n == 2 else my_rows, cols]
            return remote(
                block, block, (hsem.at[0, l, n, j], hsem.at[1, l, n, j]), x_dev if n == 0 else core_dev
            )

        def hidden_step(j, carry):
            cols = pl.ds(pl.multiple_of(j * LANES, LANES), LANES)
            x_copy(j).wait_recv()
            s = (
                part[j, my_rows, :].astype(f32)
                + crecv[l, j, m_local, :].astype(f32)
                + xrecv[l, j].astype(f32)
            )
            mixed = s[:, :LANES] + bias[l : l + 1, cols]
            hid[l, my_rows, cols] = (mixed / (1.0 + jnp.exp(-mixed)) * s[:, LANES:]).astype(bf16)
            h_copy(j, 0).start()
            h_copy(j, 1).start()
            return carry

        lax.fori_loop(0, tiles, hidden_step, 0)

        def forward_step(j, carry):
            h_copy(j, 0).wait_recv()
            h_copy(j, 2).start()
            return carry

        lax.fori_loop(0, tiles, forward_step, 0)

        def gathered_step(j, carry):
            h_copy(j, 1).wait_recv()
            h_copy(j, 2).wait_recv()
            core_copy(j).wait_send()
            x_copy(j).wait_send()
            for n in range(3):
                h_copy(j, n).wait_send()
            return carry

        lax.fori_loop(0, tiles, gathered_step, 0)

        def y_copy(k):
            zz = lax.rem(z + k, n_z)
            return remote(
                ysend.at[zr(zz), :], yrecv.at[l, zr(zz), :], (ysem.at[0, l, k - 1], ysem.at[1, l, k - 1]), y_dev
            )

        width = 256
        other_y = pl.ds(pl.multiple_of((1 - y) * half, half), half)
        own_y = pl.ds(pl.multiple_of(y * half, half), half)

        def down_other(i, carry):
            cols = pl.ds(pl.multiple_of(i * width, width), width)
            ysend[:, cols] = jnp.dot(hid[l, other_y, :], dwb[:, cols], preferred_element_type=f32).astype(bf16)
            return carry

        def down_own(i, carry):
            cols = pl.ds(pl.multiple_of(i * width, width), width)
            own[:, cols] = jnp.dot(hid[l, own_y, :], dwb[:, cols], preferred_element_type=f32)
            return carry

        lax.fori_loop(0, d_loc // width, down_other, 0)
        for k in range(1, n_z + 1):
            y_copy(k).start()
        lax.fori_loop(0, d_loc // width, down_own, 0)

        def z_copy(k):
            zz = lax.rem(z + k, n_z)
            return remote(
                zsend.at[zr(zz), :], zrecv.at[l, k - 1], (zsem.at[0, l, k - 1], zsem.at[1, l, k - 1]), z_dev(k)
            )

        for k in range(1, n_z):
            zz = lax.rem(z + k, n_z)
            y_copy(k).wait_recv()
            zsend[zr(zz), :] = (own[zr(zz), :] + yrecv[l, zr(zz), :].astype(f32)).astype(bf16)
            z_copy(k).start()
        y_copy(n_z).wait_recv()
        acc = own[zr(z), :] + yrecv[l, zr(z), :].astype(f32)
        for k in range(1, n_z):
            z_copy(k).wait_recv()
            acc = acc + zrecv[l, k - 1].astype(f32)
        mine = hr(y, z)
        new = residual_scale * h[mine, :].astype(f32) + acc * ds_[l : l + 1, :]
        hnew[l, mine, :] = new.astype(bf16)

        def gather_z(k):
            return remote(
                hnew.at[l, mine, :],
                hnew.at[l, mine, :],
                (asem.at[0, l, k - 1], asem.at[1, l, k - 1]),
                z_dev(k),
            )

        def gather_y(k):
            block = hnew.at[l, hr(y, lax.rem(z + n_z - k, n_z)), :]
            return remote(block, block, (fsem.at[0, l, k], fsem.at[1, l, k]), y_dev)

        for k in range(1, n_z):
            gather_z(k).start()
        gather_y(0).start()
        for k in range(1, n_z):
            gather_z(k).wait_recv()
            gather_y(k).start()
        for k in range(n_z):
            gather_y(k).wait_recv()
        for k in range(1, n_z + 1):
            y_copy(k).wait_send()
        for k in range(1, n_z):
            z_copy(k).wait_send()
            gather_z(k).wait_send()
        for k in range(n_z):
            gather_y(k).wait_send()
    out[...] = hnew[layers - 1]


def fused(n_ra, tokens, gate_weight, up_weight, down_weight, gate_scale, up_scale, down_scale, gain, taps, bias, d_all):
    n_tok, d_loc = tokens.shape
    layers, _, f_loc = gate_weight.shape
    n_z = n_ra // 2
    tiles = f_loc // LANES
    half, quarter = n_tok // 2, n_tok // 4
    f32, bf16 = jnp.float32, jnp.bfloat16
    dma = pltpu.SemaphoreType.DMA
    vmem, hbm = pl.BlockSpec(memory_space=pltpu.VMEM), pl.BlockSpec(memory_space=pl.ANY)
    zrows = half // n_z
    return pl.pallas_call(
        functools.partial(kernel, (layers, n_tok, d_loc, f_loc, d_all, n_z)),
        out_shape=jax.ShapeDtypeStruct((n_tok, d_loc), bf16),
        in_specs=[vmem, hbm, hbm, hbm] + [vmem] * 6,
        out_specs=vmem,
        scratch_shapes=[
            pltpu.VMEM((layers, d_loc, f_loc), f32),
            pltpu.VMEM((layers, d_loc, f_loc), f32),
            pltpu.VMEM((layers, f_loc, d_loc), f32),
            pltpu.VMEM((f_loc, d_loc), bf16),
            pltpu.VMEM((n_tok, d_loc), bf16),
            pltpu.VMEM((n_tok, LANES), f32),
            pltpu.VMEM((layers, 4, 8, LANES), f32),
            pltpu.VMEM((tiles, n_tok, 2 * LANES), bf16),
            pltpu.VMEM((layers, tiles, half, 2 * LANES), bf16),
            pltpu.VMEM((tiles, quarter, 2 * LANES), bf16),
            pltpu.VMEM((layers, tiles, quarter, 2 * LANES), bf16),
            pltpu.VMEM((layers, n_tok, f_loc), bf16),
            pltpu.VMEM((half, d_loc), bf16),
            pltpu.VMEM((half, d_loc), f32),
            pltpu.VMEM((layers, half, d_loc), bf16),
            pltpu.VMEM((half, d_loc), bf16),
            pltpu.VMEM((layers, n_z - 1, zrows, d_loc), bf16),
            pltpu.VMEM((layers, n_tok, d_loc), bf16),
            dma((layers, 3)),
            dma((2, layers, 3)),
            dma((2, layers, tiles)),
            dma((2, layers, tiles)),
            dma((2, layers, 3, tiles)),
            dma((2, layers, n_z)),
            dma((2, layers, n_z - 1)),
            dma((2, layers, n_z - 1)),
            dma((2, layers, n_z)),
        ],
        compiler_params=pltpu.CompilerParams(
            collective_id=0, has_side_effects=True, vmem_limit_bytes=67_043_328
        ),
    )(tokens, gate_weight, up_weight, down_weight, gate_scale, up_scale, down_scale, gain, taps, bias)


def plain(tokens, gate_weight, up_weight, down_weight, gate_scale, up_scale, down_scale, gain, conv_taps, bias, d_all):
    hstate = tokens
    for layer in range(gate_weight.shape[0]):
        wide = hstate.astype(jnp.float32)
        squares = jnp.sum(wide * wide, axis=1)
        operand = (wide * gain[layer]).astype(jnp.bfloat16)
        gate_part = jnp.dot(operand, gate_weight[layer].astype(jnp.bfloat16), preferred_element_type=jnp.float32)
        up_part = jnp.dot(operand, up_weight[layer].astype(jnp.bfloat16), preferred_element_type=jnp.float32)
        gate_sum, up_sum, square_sum = lax.psum((gate_part, up_part, squares), "cb")
        rscale = lax.rsqrt(square_sum / d_all + norm_eps)[:, None]
        gate = gate_sum * rscale * gate_scale[layer]
        upward = up_sum * rscale * up_scale[layer]
        padded = jnp.pad(gate, ((1, 1), (0, 0)))
        taps = conv_taps[layer]
        mixed = taps[0] * padded[:-2] + taps[1] * padded[1:-1] + taps[2] * padded[2:] + bias[layer]
        hidden = (jax.nn.silu(mixed) * upward).astype(jnp.bfloat16)
        term = jnp.dot(hidden, down_weight[layer].astype(jnp.bfloat16), preferred_element_type=jnp.float32)
        branch = lax.psum(term, "ra") * down_scale[layer]
        hstate = (residual_scale * wide + branch).astype(jnp.bfloat16)
    return hstate


def solution(mesh):
    n_ra, n_cb = mesh.shape["ra"], mesh.shape["cb"]

    def per_device(*args):
        n_tok, d_loc = args[0].shape
        f_loc = args[1].shape[2]
        fits = n_cb == 4 and n_ra % 2 == 0 and n_ra >= 4 and n_tok % (16 * n_ra) == 0 and n_tok <= 8 * LANES
        fits = fits and f_loc % LANES == 0 and d_loc % 256 == 0 and f_loc > LAG * LANES
        if fits:
            return fused(n_ra, *args, d_loc * n_cb)
        return plain(*args, d_loc * n_cb)

    in_specs = (
        P(None, "cb"),
        P(None, "cb", "ra"),
        P(None, "cb", "ra"),
        P(None, "ra", "cb"),
        P(None, "ra"),
        P(None, "ra"),
        P(None, "cb"),
        P(None, "cb"),
        P(None, None, "ra"),
        P(None, "ra"),
    )
    return jax.shard_map(
        per_device, mesh=mesh, in_specs=in_specs, out_specs=P(None, "cb"), check_vma=False
    )
```

```python
import functools

import jax
import jax.numpy as jnp
from jax import lax
from jax.experimental import pallas as pl
from jax.experimental.pallas import tpu as pltpu
from jax.sharding import PartitionSpec as P

MESH = pl.DeviceIdType.MESH
norm_eps = 1e-06
residual_scale = 0.25
LANES = 128
LAG = 3
CHUNKS = 2


def kernel(
    sizes,
    tok,
    gw_hbm,
    uw_hbm,
    dw_hbm,
    gs,
    us,
    ds_,
    gain,
    taps,
    bias,
    out,
    gw,
    uw,
    dw,
    dwb,
    operand,
    rsb,
    stat,
    part,
    crecv,
    xsend,
    xrecv,
    hid,
    ysend,
    own,
    yrecv,
    zsend,
    zrecv,
    hnew,
    wsem,
    ssem,
    csem,
    xsem,
    hsem,
    ysem,
    zsem,
    asem,
    fsem,
):
    layers, n_tok, d_loc, f_loc, d_all, n_z = sizes
    tiles = f_loc // LANES
    span = n_tok // CHUNKS
    half, quarter = span // 2, span // 4
    zrows = half // n_z
    f32, bf16 = jnp.float32, jnp.bfloat16
    ra, cb = lax.axis_index("ra"), lax.axis_index("cb")
    z, y = ra // 2, ra % 2
    x, c = cb // 2, cb % 2
    core_dev = (ra, x * 2 + (1 - c))
    x_dev = (ra, (1 - x) * 2 + c)
    y_dev = (z * 2 + (1 - y), cb)

    def z_dev(k):
        return (lax.rem(z + k, n_z) * 2 + y, cb)

    def remote(src, dst, sems, dev):
        return pltpu.make_async_remote_copy(
            src_ref=src, dst_ref=dst, send_sem=sems[0], recv_sem=sems[1], device_id=dev, device_id_type=MESH
        )

    def load(l, n):
        src, dst = ((gw_hbm, gw), (uw_hbm, uw), (dw_hbm, dw))[n]
        return pltpu.make_async_copy(src.at[l], dst.at[l], wsem.at[l, n])

    load(0, 0).start()
    load(0, 1).start()

    barrier = pltpu.get_barrier_semaphore()
    peers = [(ra, lax.rem(cb + k, 4)) for k in range(1, 4)] + [y_dev] + [z_dev(k) for k in range(1, n_z)]
    for dev in peers:
        pl.semaphore_signal(barrier, inc=1, device_id=dev, device_id_type=MESH)
    pl.semaphore_wait(barrier, len(peers))

    def block_rows(ch, cc, xx):
        return pl.ds(pl.multiple_of(ch * span + cc * half + xx * quarter, quarter), quarter)

    def zr(zz):
        return pl.ds(pl.multiple_of(zz * zrows, zrows), zrows)

    def hr(ch, yy, zz):
        return pl.ds(pl.multiple_of(ch * span + yy * half + zz * zrows, zrows), zrows)

    for l in range(layers):
        h = tok if l == 0 else hnew.at[l - 1]
        wide = h[...].astype(f32)
        ssq = jnp.sum(wide * wide, axis=1, keepdims=True)
        lane = lax.broadcasted_iota(jnp.int32, (n_tok, LANES), 1)
        row = lax.broadcasted_iota(jnp.int32, (n_tok, LANES), 0)
        pick = lane == lax.shift_right_logical(row, 3)
        packed = jnp.where(pick, jnp.broadcast_to(ssq, (n_tok, LANES)), 0.0)
        stat[l, 0] = jnp.sum(packed.reshape(n_tok // 8, 8, LANES), axis=0)
        for k in range(1, 4):
            remote(
                stat.at[l, 0], stat.at[l, k], (ssem.at[0, l, k - 1], ssem.at[1, l, k - 1]), (ra, lax.rem(cb + k, 4))
            ).start()
        operand[...] = (h[...].astype(f32) * gain[l : l + 1, :]).astype(bf16)
        if l == 0:
            load(0, 0).wait()
            load(0, 1).wait()
            load(0, 2).start()
            for ll in range(1, layers):
                for n in range(3):
                    load(ll, n).start()
        else:
            load(l, 0).wait()
            load(l, 1).wait()
        for k in range(1, 4):
            remote(
                stat.at[l, 0], stat.at[l, k], (ssem.at[0, l, k - 1], ssem.at[1, l, k - 1]), (ra, lax.rem(cb + k, 4))
            ).wait()
        total = stat[l, 0] + stat[l, 1] + stat[l, 2] + stat[l, 3]
        spread = jnp.broadcast_to(total[None], (n_tok // 8, 8, LANES)).reshape(n_tok, LANES)
        summed = jnp.sum(jnp.where(pick, spread, 0.0), axis=1, keepdims=True)
        rsb[...] = jnp.broadcast_to(lax.rsqrt(summed / d_all + norm_eps), (n_tok, LANES))

        def core_copy(ch, j):
            rows = pl.ds(pl.multiple_of(ch * span + (1 - c) * half, half), half)
            return remote(
                part.at[j, rows, :], crecv.at[l, ch, j], (csem.at[0, l, ch, j], csem.at[1, l, ch, j]), core_dev
            )

        def x_copy(ch, j):
            return remote(xsend.at[ch, j], xrecv.at[l, ch, j], (xsem.at[0, l, ch, j], xsem.at[1, l, ch, j]), x_dev)

        x_local = pl.ds(pl.multiple_of((1 - x) * quarter, quarter), quarter)
        m_local = pl.ds(pl.multiple_of(x * quarter, quarter), quarter)

        def x_step(ch, i):
            core_copy(ch, i).wait_recv()
            xsend[ch, i] = (
                part[i, block_rows(ch, c, 1 - x), :].astype(f32) + crecv[l, ch, i, x_local, :].astype(f32)
            ).astype(bf16)
            x_copy(ch, i).start()

        def gate_step(j, carry):
            @pl.when(j < tiles)
            def _():
                cols = pl.ds(pl.multiple_of(j * LANES, LANES), LANES)
                w = jnp.concatenate([gw[l, :, cols].astype(bf16), uw[l, :, cols].astype(bf16)], axis=1)
                acc = jnp.dot(operand[...], w, preferred_element_type=f32)
                rs = rsb[...]
                g = acc[:, :LANES] * rs * gs[l : l + 1, cols]
                rows = lax.broadcasted_iota(jnp.int32, g.shape, 0)
                prev = jnp.where(rows == 0, 0.0, pltpu.roll(g, 1, 0))
                nxt = jnp.where(rows == n_tok - 1, 0.0, pltpu.roll(g, n_tok - 1, 0))
                mixed = taps[l, 0:1, cols] * prev + taps[l, 1:2, cols] * g + taps[l, 2:3, cols] * nxt
                part[j, :, 0:LANES] = mixed.astype(bf16)
                part[j, :, LANES : 2 * LANES] = (acc[:, LANES:] * rs * us[l : l + 1, cols]).astype(bf16)
                for ch in range(CHUNKS):
                    core_copy(ch, j).start()

            @pl.when(j >= LAG)
            def _():
                x_step(0, j - LAG)

            return carry

        lax.fori_loop(0, tiles + LAG, gate_step, 0)

        load(l, 2).wait()

        def cast_step(i, carry):
            r = pl.ds(pl.multiple_of(i * LANES, LANES), LANES)
            dwb[r, :] = dw[l, r, :].astype(bf16)
            return carry

        lax.fori_loop(0, tiles, cast_step, 0)

        def h_copy(ch, j, n):
            cols = pl.ds(pl.multiple_of(j * LANES, LANES), LANES)
            block = hid.at[l, block_rows(ch, c, 1 - x if n == 2 else x), cols]
            return remote(
                block, block, (hsem.at[0, l, ch, n, j], hsem.at[1, l, ch, n, j]), x_dev if n == 0 else core_dev
            )

        def hidden(ch):
            my_rows = block_rows(ch, c, x)

            def step(j, carry):
                cols = pl.ds(pl.multiple_of(j * LANES, LANES), LANES)
                x_copy(ch, j).wait_recv()
                s = (
                    part[j, my_rows, :].astype(f32)
                    + crecv[l, ch, j, m_local, :].astype(f32)
                    + xrecv[l, ch, j].astype(f32)
                )
                mixed = s[:, :LANES] + bias[l : l + 1, cols]
                hid[l, my_rows, cols] = (mixed / (1.0 + jnp.exp(-mixed)) * s[:, LANES:]).astype(bf16)
                h_copy(ch, j, 0).start()
                h_copy(ch, j, 1).start()
                return carry

            lax.fori_loop(0, tiles, step, 0)

        def gather_hidden(ch):
            def forward_step(j, carry):
                h_copy(ch, j, 0).wait_recv()
                h_copy(ch, j, 2).start()
                return carry

            lax.fori_loop(0, tiles, forward_step, 0)

            def gathered_step(j, carry):
                h_copy(ch, j, 1).wait_recv()
                h_copy(ch, j, 2).wait_recv()
                return carry

            lax.fori_loop(0, tiles, gathered_step, 0)

        def y_copy(ch, k):
            zz = lax.rem(z + k, n_z)
            return remote(
                ysend.at[ch, zr(zz), :],
                yrecv.at[l, ch, zr(zz), :],
                (ysem.at[0, l, ch, k - 1], ysem.at[1, l, ch, k - 1]),
                y_dev,
            )

        def down(ch):
            width = 256
            other_y = pl.ds(pl.multiple_of(ch * span + (1 - y) * half, half), half)
            own_y = pl.ds(pl.multiple_of(ch * span + y * half, half), half)

            def down_other(i, carry):
                cols = pl.ds(pl.multiple_of(i * width, width), width)
                ysend[ch, :, cols] = jnp.dot(
                    hid[l, other_y, :], dwb[:, cols], preferred_element_type=f32
                ).astype(bf16)
                return carry

            def down_own(i, carry):
                cols = pl.ds(pl.multiple_of(i * width, width), width)
                own[ch, :, cols] = jnp.dot(hid[l, own_y, :], dwb[:, cols], preferred_element_type=f32)
                return carry

            lax.fori_loop(0, d_loc // width, down_other, 0)
            for k in range(1, n_z + 1):
                y_copy(ch, k).start()
            lax.fori_loop(0, d_loc // width, down_own, 0)

        def z_copy(ch, k):
            zz = lax.rem(z + k, n_z)
            return remote(
                zsend.at[ch, zr(zz), :],
                zrecv.at[l, ch, k - 1],
                (zsem.at[0, l, ch, k - 1], zsem.at[1, l, ch, k - 1]),
                z_dev(k),
            )

        def spread_z(ch):
            for k in range(1, n_z):
                zz = lax.rem(z + k, n_z)
                y_copy(ch, k).wait_recv()
                zsend[ch, zr(zz), :] = (own[ch, zr(zz), :] + yrecv[l, ch, zr(zz), :].astype(f32)).astype(bf16)
                z_copy(ch, k).start()

        def gather_z(ch, k):
            block = hnew.at[l, hr(ch, y, z), :]
            return remote(block, block, (asem.at[0, l, ch, k - 1], asem.at[1, l, ch, k - 1]), z_dev(k))

        def gather_y(ch, k):
            block = hnew.at[l, hr(ch, y, lax.rem(z + n_z - k, n_z)), :]
            return remote(block, block, (fsem.at[0, l, ch, k], fsem.at[1, l, ch, k]), y_dev)

        def finish(ch):
            y_copy(ch, n_z).wait_recv()
            acc = own[ch, zr(z), :] + yrecv[l, ch, zr(z), :].astype(f32)
            for k in range(1, n_z):
                z_copy(ch, k).wait_recv()
                acc = acc + zrecv[l, ch, k - 1].astype(f32)
            mine = hr(ch, y, z)
            new = residual_scale * h[mine, :].astype(f32) + acc * ds_[l : l + 1, :]
            hnew[l, mine, :] = new.astype(bf16)
            for k in range(1, n_z):
                gather_z(ch, k).start()
            gather_y(ch, 0).start()

        def forward(ch):
            for k in range(1, n_z):
                gather_z(ch, k).wait_recv()
                gather_y(ch, k).start()

        def second_x(i, carry):
            x_step(1, i)
            return carry

        hidden(0)
        lax.fori_loop(0, tiles, second_x, 0)
        gather_hidden(0)
        down(0)
        spread_z(0)
        hidden(1)
        finish(0)
        gather_hidden(1)
        down(1)
        forward(0)
        spread_z(1)
        finish(1)
        forward(1)
        for ch in range(CHUNKS):
            for k in range(n_z):
                gather_y(ch, k).wait_recv()

        for ch in range(CHUNKS):

            def sent_step(j, carry, ch=ch):
                core_copy(ch, j).wait_send()
                x_copy(ch, j).wait_send()
                for n in range(3):
                    h_copy(ch, j, n).wait_send()
                return carry

            lax.fori_loop(0, tiles, sent_step, 0)
            for k in range(1, n_z + 1):
                y_copy(ch, k).wait_send()
            for k in range(1, n_z):
                z_copy(ch, k).wait_send()
                gather_z(ch, k).wait_send()
            for k in range(n_z):
                gather_y(ch, k).wait_send()
    out[...] = hnew[layers - 1]


def fused(n_ra, tokens, gate_weight, up_weight, down_weight, gate_scale, up_scale, down_scale, gain, taps, bias, d_all):
    n_tok, d_loc = tokens.shape
    layers, _, f_loc = gate_weight.shape
    n_z = n_ra // 2
    tiles = f_loc // LANES
    half, quarter = n_tok // CHUNKS // 2, n_tok // CHUNKS // 4
    f32, bf16 = jnp.float32, jnp.bfloat16
    dma = pltpu.SemaphoreType.DMA
    vmem, hbm = pl.BlockSpec(memory_space=pltpu.VMEM), pl.BlockSpec(memory_space=pl.ANY)
    zrows = half // n_z
    return pl.pallas_call(
        functools.partial(kernel, (layers, n_tok, d_loc, f_loc, d_all, n_z)),
        out_shape=jax.ShapeDtypeStruct((n_tok, d_loc), bf16),
        in_specs=[vmem, hbm, hbm, hbm] + [vmem] * 6,
        out_specs=vmem,
        scratch_shapes=[
            pltpu.VMEM((layers, d_loc, f_loc), f32),
            pltpu.VMEM((layers, d_loc, f_loc), f32),
            pltpu.VMEM((layers, f_loc, d_loc), f32),
            pltpu.VMEM((f_loc, d_loc), bf16),
            pltpu.VMEM((n_tok, d_loc), bf16),
            pltpu.VMEM((n_tok, LANES), f32),
            pltpu.VMEM((layers, 4, 8, LANES), f32),
            pltpu.VMEM((tiles, n_tok, 2 * LANES), bf16),
            pltpu.VMEM((layers, CHUNKS, tiles, half, 2 * LANES), bf16),
            pltpu.VMEM((CHUNKS, tiles, quarter, 2 * LANES), bf16),
            pltpu.VMEM((layers, CHUNKS, tiles, quarter, 2 * LANES), bf16),
            pltpu.VMEM((layers, n_tok, f_loc), bf16),
            pltpu.VMEM((CHUNKS, half, d_loc), bf16),
            pltpu.VMEM((CHUNKS, half, d_loc), f32),
            pltpu.VMEM((layers, CHUNKS, half, d_loc), bf16),
            pltpu.VMEM((CHUNKS, half, d_loc), bf16),
            pltpu.VMEM((layers, CHUNKS, n_z - 1, zrows, d_loc), bf16),
            pltpu.VMEM((layers, n_tok, d_loc), bf16),
            dma((layers, 3)),
            dma((2, layers, 3)),
            dma((2, layers, CHUNKS, tiles)),
            dma((2, layers, CHUNKS, tiles)),
            dma((2, layers, CHUNKS, 3, tiles)),
            dma((2, layers, CHUNKS, n_z)),
            dma((2, layers, CHUNKS, n_z - 1)),
            dma((2, layers, CHUNKS, n_z - 1)),
            dma((2, layers, CHUNKS, n_z)),
        ],
        compiler_params=pltpu.CompilerParams(
            collective_id=0, has_side_effects=True, vmem_limit_bytes=67_043_328
        ),
    )(tokens, gate_weight, up_weight, down_weight, gate_scale, up_scale, down_scale, gain, taps, bias)


def plain(tokens, gate_weight, up_weight, down_weight, gate_scale, up_scale, down_scale, gain, conv_taps, bias, d_all):
    hstate = tokens
    for layer in range(gate_weight.shape[0]):
        wide = hstate.astype(jnp.float32)
        squares = jnp.sum(wide * wide, axis=1)
        operand = (wide * gain[layer]).astype(jnp.bfloat16)
        gate_part = jnp.dot(operand, gate_weight[layer].astype(jnp.bfloat16), preferred_element_type=jnp.float32)
        up_part = jnp.dot(operand, up_weight[layer].astype(jnp.bfloat16), preferred_element_type=jnp.float32)
        gate_sum, up_sum, square_sum = lax.psum((gate_part, up_part, squares), "cb")
        rscale = lax.rsqrt(square_sum / d_all + norm_eps)[:, None]
        gate = gate_sum * rscale * gate_scale[layer]
        upward = up_sum * rscale * up_scale[layer]
        padded = jnp.pad(gate, ((1, 1), (0, 0)))
        taps = conv_taps[layer]
        mixed = taps[0] * padded[:-2] + taps[1] * padded[1:-1] + taps[2] * padded[2:] + bias[layer]
        hidden = (jax.nn.silu(mixed) * upward).astype(jnp.bfloat16)
        term = jnp.dot(hidden, down_weight[layer].astype(jnp.bfloat16), preferred_element_type=jnp.float32)
        branch = lax.psum(term, "ra") * down_scale[layer]
        hstate = (residual_scale * wide + branch).astype(jnp.bfloat16)
    return hstate


def solution(mesh):
    n_ra, n_cb = mesh.shape["ra"], mesh.shape["cb"]

    def per_device(*args):
        n_tok, d_loc = args[0].shape
        f_loc = args[1].shape[2]
        fits = n_cb == 4 and n_ra % 2 == 0 and n_ra >= 4 and n_tok % (16 * CHUNKS * n_ra) == 0 and n_tok <= 8 * LANES
        fits = fits and f_loc % LANES == 0 and d_loc % 256 == 0 and f_loc > LAG * LANES
        if fits:
            return fused(n_ra, *args, d_loc * n_cb)
        return plain(*args, d_loc * n_cb)

    in_specs = (
        P(None, "cb"),
        P(None, "cb", "ra"),
        P(None, "cb", "ra"),
        P(None, "ra", "cb"),
        P(None, "ra"),
        P(None, "ra"),
        P(None, "cb"),
        P(None, "cb"),
        P(None, None, "ra"),
        P(None, "ra"),
    )
    return jax.shard_map(
        per_device, mesh=mesh, in_specs=in_specs, out_specs=P(None, "cb"), check_vma=False
    )
```
